32 devices in a mesh: fs: 8 (over z, y), tp: 4 (over x, core).
Axes of the slice: x: 2, y: 2, z: 4, core: 2. Of those that a mesh axis runs over, the one named last changes fastest.
Arguments:
- tokens: bfloat16 [3072, 2048], P('fs'), may hold values from -6 to 6
- norm_gain: float32 [2048], replicated, may hold values from 0.1 to 1.9
- w_gate: bfloat16 [2048, 4096], P('fs', 'tp'), may hold values from -0.125 to 0.125
- w_up: bfloat16 [2048, 4096], P('fs', 'tp'), may hold values from -0.125 to 0.125
- w_down: bfloat16 [4096, 2048], P('tp', 'fs'), may hold values from -0.09375 to 0.09375
- cotangent: bfloat16 [3072, 2048], P('fs'), may hold values from -6 to 6
Outputs:
- grad_tokens: bfloat16 [3072, 2048], P('fs')
- grad_down: float32 [4096, 2048], P('tp', 'fs')
- down_norms: float32 [4096], P('tp')
The draws below stay inside these ranges and needn't reach their ends.
All inputs are finite; a program needn't handle non-finite values.
Results may differ from the reference program's by a relative error of at most 0.018.
Values may be sent and summed in bfloat16 or wider, within the bound.
A program may use at most 64 MiB of HBM per device.

```python
import jax
import jax.numpy as jnp
from jax import lax

D = 2048
FF = 4096
TOKENS = 3072
N_TP = 4


def spiked(drawn, rng, source, target, blocks, factor):
    def block_of(position):
        return (jnp.arange(drawn.shape[position]) // (drawn.shape[position] // blocks)).reshape((-1,) + (1,) * (drawn.ndim - 1 - position))

    first = jax.random.permutation(rng, blocks)[block_of(target)]
    other_side = (block_of(target) + blocks // 2) % blocks
    return jnp.where((block_of(source) == first) | (block_of(source) == other_side), factor * drawn, drawn)


def steps_of(key, extent, cuts, least, largest):
    level = 1.0
    for position, blocks in cuts:
        heights = jax.random.uniform(jax.random.fold_in(jax.random.fold_in(key, 6), position), (blocks,), jnp.float32, least / len(cuts), largest / len(cuts))
        level = level * jnp.repeat(jnp.exp(heights), extent[position] // blocks).reshape((-1,) + (1,) * (len(extent) - 1 - position))
    return level


def noise(stream_key, shape, scale, limit, pieces=(), kind=jnp.bfloat16):
    loudness = steps_of(stream_key, shape, pieces, -0.22, 0.18) if pieces else 1.0
    array = jax.random.normal(stream_key, shape, jnp.float32) * scale * loudness
    return jnp.minimum(jnp.maximum(array, -limit), limit).astype(kind)


def bell_draw_with(own_key, extent, scale, bound, cuts, heavy, held_as=jnp.bfloat16):
    values = scale * jax.random.normal(own_key, extent, jnp.float32)
    if cuts:
        values = values * steps_of(own_key, extent, cuts, -0.22, 0.18)
    return jnp.clip(spiked(values, jax.random.fold_in(own_key, 3), *heavy), -bound, bound).astype(held_as)


def setup_inputs(seed: int = 0) -> dict:
    key_list = jax.random.split(jax.random.key(seed), 7)
    tokens = noise(key_list[0], (TOKENS, D), 1.0, 6.0, ((0, 8),))
    norm_gain = jnp.clip(1.0 + 0.18 * jax.random.normal(key_list[1], (D,), jnp.float32), 0.1, 1.9)
    w_gate = noise(key_list[2], (D, FF), D ** -0.5, 0.125, ((0, 8), (1, 4)))
    w_up = noise(key_list[3], (D, FF), D ** -0.5, 0.125, ((0, 8), (1, 4)))
    w_down = noise(key_list[4], (FF, D), FF ** -0.5, 0.09375, ((0, 4), (1, 8)))
    cotangent = bell_draw_with(key_list[5], (TOKENS, D), 1.0, 6.0, ((0, 8),), (0, 1, 8, 2.0))
    return dict(tokens=tokens, norm_gain=norm_gain, w_gate=w_gate, w_up=w_up, w_down=w_down, cotangent=cotangent)


EPS = 1e-06

def reference(tokens, norm_gain, w_gate, w_up, w_down, cotangent):
    xf = tokens.astype(jnp.float32)
    inv = lax.rsqrt(lax.optimization_barrier(jnp.mean(xf * xf, axis=-1, keepdims=True)) + EPS)
    scaled = xf * inv
    normed = (scaled * norm_gain).astype(jnp.bfloat16)
    gate = jnp.dot(normed, w_gate, preferred_element_type=jnp.float32)
    up = jnp.dot(normed, w_up, preferred_element_type=jnp.float32)
    sig = jax.nn.sigmoid(gate)
    act = gate * sig
    hidden = (act * up).astype(jnp.bfloat16)
    d_hidden = 0.5 * lax.dot_general(cotangent, w_down, (((1,), (1,)), ((), ())), preferred_element_type=jnp.float32)
    grad_down = 0.5 * lax.dot_general(hidden, cotangent, (((0,), (0,)), ((), ())), preferred_element_type=jnp.float32)
    down_norms = lax.optimization_barrier(jnp.sum(grad_down * grad_down, axis=1))
    d_gate = (d_hidden * up * sig * (1.0 + gate * (1.0 - sig))).astype(jnp.bfloat16)
    d_up = (d_hidden * act).astype(jnp.bfloat16)
    width = FF // N_TP

    def block(total, index):
        start = (index * width).astype(jnp.int32)
        gate_part = lax.dynamic_slice_in_dim(d_gate, start, width, 1)
        up_part = lax.dynamic_slice_in_dim(d_up, start, width, 1)
        gate_rows = lax.dynamic_slice_in_dim(w_gate, start, width, 1)
        up_rows = lax.dynamic_slice_in_dim(w_up, start, width, 1)
        part = lax.dot_general(gate_part, gate_rows, (((1,), (1,)), ((), ())), preferred_element_type=jnp.float32)
        part = part + lax.dot_general(up_part, up_rows, (((1,), (1,)), ((), ())), preferred_element_type=jnp.float32)
        rounded = lax.optimization_barrier(part.astype(jnp.bfloat16))
        return (total + rounded.astype(jnp.float32), None)
    start_total = jnp.zeros(tokens.shape, jnp.float32)
    d_normed, unused = lax.scan(block, start_total, jnp.arange(N_TP, dtype=jnp.int32))
    d_scaled = d_normed * norm_gain
    inner = lax.optimization_barrier(jnp.mean(d_scaled * scaled, axis=-1, keepdims=True))
    grad_tokens = (inv * (d_scaled - scaled * inner)).astype(jnp.bfloat16)
    return (grad_tokens, grad_down, down_norms)
```

```python
import functools

import jax
import jax.numpy as jnp
from jax import lax
from jax.sharding import PartitionSpec as P

EPS = 1e-06
BF16 = jnp.bfloat16
F32 = jnp.float32


def place(pieces, count):
    first = pieces[0][1]
    held = jnp.zeros((count,) + first.shape, first.dtype)
    for position, piece in pieces:
        held = lax.dynamic_update_slice_in_dim(held, piece[None], position, 0)
    return held


def take(array, position, axis=0):
    return lax.dynamic_index_in_dim(array, position, axis, keepdims=False)


def shards(n_fs, n_tp, tokens, norm_gain, w_gate, w_up, w_down, cotangent):
    n_y = 2 ** ((n_fs.bit_length() - 1) // 2)
    n_z, n_x = n_fs // n_y, n_tp // 2
    n_q = n_z // 2
    f, t = lax.axis_index("fs"), lax.axis_index("tp")
    z, y, x, c = f // n_y, f % n_y, t // 2, t % 2
    q, h = z // 2, z % 2
    rows, d_model = tokens.shape
    depth, half = w_gate.shape[0], w_gate.shape[1] // 2
    piece = rows // n_tp

    def to_z(a, step):
        return lax.ppermute(a, "fs", [(i, (i + step * n_y) % n_fs) for i in range(n_fs)])

    def to_y(a, step):
        return lax.ppermute(
            a, "fs", [(i, i // n_y * n_y + (i + step) % n_y) for i in range(n_fs)]
        )

    def to_twin(a):
        return lax.ppermute(
            a, "fs", [(i, (i // n_y ^ 1) * n_y + i % n_y) for i in range(n_fs)]
        )

    def to_x(a, step):
        return lax.ppermute(a, "tp", [(i, (i + 2 * step) % n_tp) for i in range(n_tp)])

    def to_core(a):
        return lax.ppermute(a, "tp", [(i, i ^ 1) for i in range(n_tp)])

    mine = jnp.stack(
        [lax.dynamic_slice_in_dim(a, t * piece, piece, 0) for a in (tokens, cotangent)]
    )
    got = to_twin(mine)
    got = place(
        [(x, got)] + [((x - s) % n_x, to_x(got, s)) for s in range(1, n_x)], n_x
    )
    got = place([(c, got), (1 - c, to_core(got))], 2)
    got = got.transpose(2, 1, 0, 3, 4).reshape(2, rows, d_model)
    tokens2 = jnp.concatenate([tokens, got[0]], axis=0)
    cot2 = jnp.concatenate([cotangent, got[1]], axis=0)

    down_t = w_down.T

    def half_of(which):
        gate_up = jnp.concatenate(
            [lax.dynamic_slice_in_dim(w, which * half, half, 1) for w in (w_gate, w_up)], axis=1
        )
        return gate_up, lax.dynamic_slice_in_dim(down_t, which * half, half, 1)

    own, other = half_of(h), half_of(1 - h)

    def gathered(which):
        pieces = []
        order = sorted(range(n_z), key=lambda s: min(s, n_z - s))
        for s in order:
            block = own[which] if s == 0 else to_z((own, other)[s % 2][which], s)
            from_z = (z - s) % n_z
            pieces.append((from_z * n_y + y, block))
            for r in range(1, n_y):
                pieces.append((from_z * n_y + (y - r) % n_y, to_y(block, r)))
        return place(pieces, n_fs).reshape(d_model, -1)

    w_gu, w_dn = gathered(0), gathered(1)

    xf = tokens2.astype(F32)
    inv = lax.rsqrt(jnp.mean(xf * xf, axis=-1, keepdims=True) + EPS)
    normed = (xf * inv * norm_gain).astype(BF16)
    gate_up = jnp.dot(normed, w_gu, preferred_element_type=F32)
    gate, up = gate_up[:, :half], gate_up[:, half:]
    sig = jax.nn.sigmoid(gate)
    act = gate * sig
    hidden = (act * up).astype(BF16)

    share = 0.5 * lax.dot_general(
        cot2, hidden, (((0,), (0,)), ((), ())), preferred_element_type=F32
    )
    share = share.reshape(n_z, n_y, depth, half)
    total = take(share, y, 1)
    for s in range(1, n_y):
        total = total + to_y(take(share, (y + s) % n_y, 1).astype(BF16), s).astype(F32)
    pairs = total.reshape(n_q, 2, depth, half)
    total = take(pairs, q)
    for s in range(1, n_q):
        total = total + to_z(take(pairs, (q + s) % n_q).astype(BF16), 2 * s).astype(F32)
    kept = take(total, h)
    came = to_twin(take(total, 1 - h).astype(BF16)).astype(F32)
    grad_down = place([(h, kept.T), (1 - h, came.T)], 2).reshape(2 * half, depth)
    norms = jnp.sum(grad_down * grad_down, axis=1)
    norms = sum([to_y(norms, s) for s in range(1, n_y)], norms)
    down_norms = sum([to_z(norms, s) for s in range(1, n_z)], norms)

    d_hidden = 0.5 * jnp.dot(cot2, w_dn, preferred_element_type=F32)
    d_gate = (d_hidden * up * sig * (1.0 + gate * (1.0 - sig))).astype(BF16)
    d_up = (d_hidden * act).astype(BF16)
    d_both = jnp.concatenate([d_gate, d_up], axis=1)
    part = lax.dot_general(
        d_both, w_gu, (((1,), (1,)), ((), ())), preferred_element_type=F32
    )
    part = part.astype(BF16).reshape(2, n_x, 2, piece, d_model)
    part = take(part, c, 2).astype(F32) + to_core(take(part, 1 - c, 2)).astype(F32)
    total = take(part, x, 1)
    for s in range(1, n_x):
        total = total + to_x(take(part, (x + s) % n_x, 1).astype(BF16), s).astype(F32)
    d_normed = total[0] + to_twin(total[1].astype(BF16)).astype(F32)

    xp = lax.dynamic_slice_in_dim(tokens, t * piece, piece, 0).astype(F32)
    inv_p = lax.rsqrt(jnp.mean(xp * xp, axis=-1, keepdims=True) + EPS)
    scaled = xp * inv_p
    d_scaled = d_normed * norm_gain
    inner = jnp.mean(d_scaled * scaled, axis=-1, keepdims=True)
    grad = (inv_p * (d_scaled - scaled * inner)).astype(BF16)
    grad = place([(x, grad)] + [((x - s) % n_x, to_x(grad, s)) for s in range(1, n_x)], n_x)
    grad = place([(c, grad), (1 - c, to_core(grad))], 2)
    grad_tokens = grad.transpose(1, 0, 2, 3).reshape(rows, d_model)
    return (grad_tokens, grad_down, down_norms)


def solution(mesh):
    in_specs = (P("fs", None), P(), P("fs", "tp"), P("fs", "tp"), P("tp", "fs"), P("fs", None))
    out_specs = (P("fs", None), P("tp", "fs"), P("tp"))
    return jax.shard_map(
        functools.partial(shards, mesh.shape["fs"], mesh.shape["tp"]),
        mesh=mesh, in_specs=in_specs, out_specs=out_specs, check_vma=False,
    )
```

```python
import functools

import jax
import jax.numpy as jnp
from jax import lax
from jax.experimental import pallas as pl
from jax.experimental.pallas import tpu as pltpu
from jax.sharding import PartitionSpec as P

EPS = 1e-06
BF16 = jnp.bfloat16
F32 = jnp.float32


def place(pieces, count):
    first = pieces[0][1]
    held = jnp.zeros((count,) + first.shape, first.dtype)
    for position, piece in pieces:
        held = lax.dynamic_update_slice_in_dim(held, piece[None], position, 0)
    return held


def take(array, position, axis=0):
    return lax.dynamic_index_in_dim(array, position, axis, keepdims=False)


def gather_kernel(n_z, n_y, n_x, own_gu, own_dn, other_gu, other_dn, mine, w_gu, w_dn, got,
                  z_send, z_recv, y_send, y_recv, x_send, x_recv, c_send, c_recv, local):
    f, t = lax.axis_index("fs"), lax.axis_index("tp")
    z, y, x, c = lax.div(f, n_y), lax.rem(f, n_y), lax.div(t, 2), lax.rem(t, 2)
    n_tp = 2 * n_x
    sources = ((own_gu, other_gu), (own_dn, other_dn))
    held = (w_gu, w_dn)

    def at_z(s):
        return {"fs": lax.rem(z + s, n_z) * n_y + y}

    def at_y(r):
        return {"fs": z * n_y + lax.rem(y + r, n_y)}

    def at_x(s):
        return {"tp": lax.rem(t + 2 * s, n_tp)}

    twin = {"fs": (z + 1 - 2 * lax.rem(z, 2)) * n_y + y}
    core = {"tp": t + 1 - 2 * c}

    barrier = pltpu.get_barrier_semaphore()
    friends = [at_z(s) for s in range(1, n_z)] + [at_y(r) for r in range(1, n_y)]
    friends += [at_x(s) for s in range(1, n_x)] + [core]
    for friend in friends:
        pl.semaphore_signal(barrier, inc=1, device_id=friend, device_id_type=pl.DeviceIdType.MESH)
    pl.semaphore_wait(barrier, len(friends))

    started = []

    def send(src, dst, out_sem, in_sem, to):
        copy = pltpu.make_async_remote_copy(
            src_ref=src, dst_ref=dst, send_sem=out_sem, recv_sem=in_sem,
            device_id=to, device_id_type=pl.DeviceIdType.MESH,
        )
        copy.start()
        started.append(copy)
        return copy

    order = sorted(range(1, n_z), key=lambda s: min(s, n_z - s))
    from_z = {}

    def start_z(k):
        for s in order:
            from_z[k, s] = send(
                sources[k][s % 2], held[k].at[f], z_send.at[k, s], z_recv.at[k, s], at_z(s)
            )

    late = []

    def forward(k, s):
        if s == 0:
            src = sources[k][0]
            slot = f
        else:
            from_z[k, s].wait_recv()
            slot = lax.rem(z + n_z - s, n_z) * n_y + y
            src = held[k].at[slot]
        for r in range(1, n_y):
            late.append(send(
                src, held[k].at[slot], y_send.at[k, s, r], y_recv.at[k, s, r], at_y(r)
            ))

    start_z(0)
    forward(0, 0)
    tokens = send(mine, got.at[:, x, c], x_send.at[0], x_recv.at[0], twin)
    start_z(1)
    forward(1, 0)
    stays = [pltpu.make_async_copy(sources[k][0], held[k].at[f], local.at[k]) for k in range(2)]
    for copy in stays:
        copy.start()
    for s in order:
        forward(0, s)
    tokens.wait_recv()
    across = [
        send(got.at[:, x, c], got.at[:, x, c], x_send.at[s], x_recv.at[s], at_x(s))
        for s in range(1, n_x)
    ]
    for s in order[:-1]:
        forward(1, s)
    for copy in across:
        copy.wait_recv()
    late.append(send(got.at[:, :, c], got.at[:, :, c], c_send, c_recv, core))
    forward(1, order[-1])
    for copy in late:
        copy.wait_recv()
    for copy in started:
        copy.wait_send()
    for copy in stays:
        copy.wait()


def gather_all(n_z, n_y, n_x, own, other, mine):
    n_fs = n_z * n_y
    dma = pltpu.SemaphoreType.DMA
    anywhere = pl.BlockSpec(memory_space=pl.ANY)
    return pl.pallas_call(
        functools.partial(gather_kernel, n_z, n_y, n_x),
        out_shape=[jax.ShapeDtypeStruct((n_fs,) + a.shape, a.dtype) for a in own]
        + [jax.ShapeDtypeStruct((2, n_x, 2) + mine.shape[1:], mine.dtype)],
        in_specs=[anywhere] * 5,
        out_specs=[anywhere] * 3,
        scratch_shapes=[
            dma((2, n_z)), dma((2, n_z)), dma((2, n_z, n_y)), dma((2, n_z, n_y)),
            dma((n_x,)), dma((n_x,)), dma, dma, dma((2,)),
        ],
        compiler_params=pltpu.CompilerParams(collective_id=0, has_side_effects=True),
    )(*own, *other, mine)


def shards(n_fs, n_tp, tokens, norm_gain, w_gate, w_up, w_down, cotangent):
    n_y = 2 ** ((n_fs.bit_length() - 1) // 2)
    n_z, n_x = n_fs // n_y, n_tp // 2
    n_q = n_z // 2
    f, t = lax.axis_index("fs"), lax.axis_index("tp")
    z, y, x, c = f // n_y, f % n_y, t // 2, t % 2
    q, h = z // 2, z % 2
    rows, d_model = tokens.shape
    depth, half = w_gate.shape[0], w_gate.shape[1] // 2
    piece = rows // n_tp

    def to_z(a, step):
        return lax.ppermute(a, "fs", [(i, (i + step * n_y) % n_fs) for i in range(n_fs)])

    def to_y(a, step):
        return lax.ppermute(
            a, "fs", [(i, i // n_y * n_y + (i + step) % n_y) for i in range(n_fs)]
        )

    def to_twin(a):
        return lax.ppermute(
            a, "fs", [(i, (i // n_y ^ 1) * n_y + i % n_y) for i in range(n_fs)]
        )

    def to_x(a, step):
        return lax.ppermute(a, "tp", [(i, (i + 2 * step) % n_tp) for i in range(n_tp)])

    def to_core(a):
        return lax.ppermute(a, "tp", [(i, i ^ 1) for i in range(n_tp)])

    mine = jnp.stack(
        [lax.dynamic_slice_in_dim(a, t * piece, piece, 0) for a in (tokens, cotangent)]
    )
    down_t = w_down.T

    def half_of(which):
        gate_up = jnp.concatenate(
            [lax.dynamic_slice_in_dim(w, which * half, half, 1) for w in (w_gate, w_up)], axis=1
        )
        return gate_up, lax.dynamic_slice_in_dim(down_t, which * half, half, 1)

    own, other = half_of(h), half_of(1 - h)

    w_gu, w_dn, got = gather_all(n_z, n_y, n_x, own, other, mine)
    w_gu, w_dn = w_gu.reshape(d_model, 2 * half), w_dn.reshape(d_model, half)
    got = got.reshape(2, rows, d_model)
    tokens2 = jnp.concatenate([tokens, got[0]], axis=0)
    cot2 = jnp.concatenate([cotangent, got[1]], axis=0)

    xf = tokens2.astype(F32)
    inv = lax.rsqrt(jnp.mean(xf * xf, axis=-1, keepdims=True) + EPS)
    normed = (xf * inv * norm_gain).astype(BF16)
    gate_up = jnp.dot(normed, w_gu, preferred_element_type=F32)
    gate, up = gate_up[:, :half], gate_up[:, half:]
    sig = jax.nn.sigmoid(gate)
    act = gate * sig
    hidden = (act * up).astype(BF16)

    share = 0.5 * lax.dot_general(
        cot2, hidden, (((0,), (0,)), ((), ())), preferred_element_type=F32
    )
    share = share.reshape(n_q, 2, n_y, depth, half)
    share, w_dn = lax.optimization_barrier((share, w_dn))

    def over_y(pair):
        block = take(share, pair)
        sent = [to_y(take(block, (y + s) % n_y, 1).astype(BF16), s) for s in range(1, n_y)]
        return sum([a.astype(F32) for a in sent], take(block, y, 1))

    away = [to_z(over_y((q + s) % n_q).astype(BF16), 2 * s) for s in range(1, n_q)]
    total = over_y(q)
    total = sum([a.astype(F32) for a in away], total)
    kept = take(total, h)
    came = to_twin(take(total, 1 - h).astype(BF16)).astype(F32)
    grad_down = place([(h, kept.T), (1 - h, came.T)], 2).reshape(2 * half, depth)
    norms = jnp.sum(grad_down * grad_down, axis=1)
    norms = sum([to_y(norms, s) for s in range(1, n_y)], norms)
    down_norms = sum([to_z(norms, s) for s in range(1, n_z)], norms)

    d_hidden = 0.5 * jnp.dot(cot2, w_dn, preferred_element_type=F32)
    d_gate = (d_hidden * up * sig * (1.0 + gate * (1.0 - sig))).astype(BF16)
    d_up = (d_hidden * act).astype(BF16)
    d_both = jnp.concatenate([d_gate, d_up], axis=1)
    part = lax.dot_general(
        d_both, w_gu, (((1,), (1,)), ((), ())), preferred_element_type=F32
    )
    part = part.astype(BF16).reshape(2, n_x, 2, piece, d_model)
    part = take(part, c, 2).astype(F32) + to_core(take(part, 1 - c, 2)).astype(F32)
    total = take(part, x, 1)
    for s in range(1, n_x):
        total = total + to_x(take(part, (x + s) % n_x, 1).astype(BF16), s).astype(F32)
    d_normed = total[0] + to_twin(total[1].astype(BF16)).astype(F32)

    xp = lax.dynamic_slice_in_dim(tokens, t * piece, piece, 0).astype(F32)
    inv_p = lax.rsqrt(jnp.mean(xp * xp, axis=-1, keepdims=True) + EPS)
    scaled = xp * inv_p
    d_scaled = d_normed * norm_gain
    inner = jnp.mean(d_scaled * scaled, axis=-1, keepdims=True)
    grad = (inv_p * (d_scaled - scaled * inner)).astype(BF16)
    grad = place([(x, grad)] + [((x - s) % n_x, to_x(grad, s)) for s in range(1, n_x)], n_x)
    grad = place([(c, grad), (1 - c, to_core(grad))], 2)
    grad_tokens = grad.transpose(1, 0, 2, 3).reshape(rows, d_model)
    return (grad_tokens, grad_down, down_norms)


def solution(mesh):
    in_specs = (P("fs", None), P(), P("fs", "tp"), P("fs", "tp"), P("tp", "fs"), P("fs", None))
    out_specs = (P("fs", None), P("tp", "fs"), P("tp"))
    return jax.shard_map(
        functools.partial(shards, mesh.shape["fs"], mesh.shape["tp"]),
        mesh=mesh, in_specs=in_specs, out_specs=out_specs, check_vma=False,
    )
```

```python
import functools

import jax
import jax.numpy as jnp
from jax import lax
from jax.experimental import pallas as pl
from jax.experimental.pallas import tpu as pltpu
from jax.sharding import PartitionSpec as P

EPS = 1e-06
BF16 = jnp.bfloat16
F32 = jnp.float32


def place(pieces, count):
    first = pieces[0][1]
    held = jnp.zeros((count,) + first.shape, first.dtype)
    for position, piece in pieces:
        held = lax.dynamic_update_slice_in_dim(held, piece[None], position, 0)
    return held


def take(array, position, axis=0):
    return lax.dynamic_index_in_dim(array, position, axis, keepdims=False)


def gather_kernel(n_z, n_y, n_x, own_gu, own_dn, other_gu, other_dn, mine, w_gu, w_dn, got,
                  z_send, z_recv, y_send, y_recv, x_send, x_recv, c_send, c_recv, local):
    f, t = lax.axis_index("fs"), lax.axis_index("tp")
    z, y, x, c = lax.div(f, n_y), lax.rem(f, n_y), lax.div(t, 2), lax.rem(t, 2)
    n_tp = 2 * n_x
    sources = ((own_gu, other_gu), (own_dn, other_dn))
    held = (w_gu, w_dn)

    def at_z(s):
        return {"fs": lax.rem(z + s, n_z) * n_y + y}

    def at_y(r):
        return {"fs": z * n_y + lax.rem(y + r, n_y)}

    def at_x(s):
        return {"tp": lax.rem(t + 2 * s, n_tp)}

    twin = {"fs": (z + 1 - 2 * lax.rem(z, 2)) * n_y + y}
    core = {"tp": t + 1 - 2 * c}

    barrier = pltpu.get_barrier_semaphore()
    friends = [at_z(s) for s in range(1, n_z)] + [at_y(r) for r in range(1, n_y)]
    friends += [at_x(s) for s in range(1, n_x)] + [core]
    for friend in friends:
        pl.semaphore_signal(barrier, inc=1, device_id=friend, device_id_type=pl.DeviceIdType.MESH)
    pl.semaphore_wait(barrier, len(friends))

    started = []

    def send(src, dst, out_sem, in_sem, to):
        copy = pltpu.make_async_remote_copy(
            src_ref=src, dst_ref=dst, send_sem=out_sem, recv_sem=in_sem,
            device_id=to, device_id_type=pl.DeviceIdType.MESH,
        )
        copy.start()
        started.append(copy)
        return copy

    order = sorted(range(1, n_z), key=lambda s: min(s, n_z - s))
    from_z = {}

    def start_z(k):
        for s in order:
            from_z[k, s] = send(
                sources[k][s % 2], held[k].at[f], z_send.at[k, s], z_recv.at[k, s], at_z(s)
            )

    late = []

    def forward(k, s):
        if s == 0:
            src = sources[k][0]
            slot = f
        else:
            from_z[k, s].wait_recv()
            slot = lax.rem(z + n_z - s, n_z) * n_y + y
            src = held[k].at[slot]
        for r in range(1, n_y):
            late.append(send(
                src, held[k].at[slot], y_send.at[k, s, r], y_recv.at[k, s, r], at_y(r)
            ))

    start_z(0)
    forward(0, 0)
    tokens = send(mine, got.at[:, x, c], x_send.at[0], x_recv.at[0], twin)
    start_z(1)
    forward(1, 0)
    stays = [pltpu.make_async_copy(sources[k][0], held[k].at[f], local.at[k]) for k in range(2)]
    for copy in stays:
        copy.start()
    for s in order:
        forward(0, s)
    tokens.wait_recv()
    across = [
        send(got.at[:, x, c], got.at[:, x, c], x_send.at[s], x_recv.at[s], at_x(s))
        for s in range(1, n_x)
    ]
    for s in order[:-1]:
        forward(1, s)
    for copy in across:
        copy.wait_recv()
    late.append(send(got.at[:, :, c], got.at[:, :, c], c_send, c_recv, core))
    forward(1, order[-1])
    for copy in late:
        copy.wait_recv()
    for copy in started:
        copy.wait_send()
    for copy in stays:
        copy.wait()


def gather_all(n_z, n_y, n_x, own, other, mine):
    n_fs = n_z * n_y
    dma = pltpu.SemaphoreType.DMA
    anywhere = pl.BlockSpec(memory_space=pl.ANY)
    return pl.pallas_call(
        functools.partial(gather_kernel, n_z, n_y, n_x),
        out_shape=[jax.ShapeDtypeStruct((n_fs,) + a.shape, a.dtype) for a in own]
        + [jax.ShapeDtypeStruct((2, n_x, 2) + mine.shape[1:], mine.dtype)],
        in_specs=[anywhere] * 5,
        out_specs=[anywhere] * 3,
        scratch_shapes=[
            dma((2, n_z)), dma((2, n_z)), dma((2, n_z, n_y)), dma((2, n_z, n_y)),
            dma((n_x,)), dma((n_x,)), dma, dma, dma((2,)),
        ],
        compiler_params=pltpu.CompilerParams(collective_id=0, has_side_effects=True),
    )(*own, *other, mine)


def shards(n_fs, n_tp, tokens, norm_gain, w_gate, w_up, w_down, cotangent):
    n_y = 2 ** ((n_fs.bit_length() - 1) // 2)
    n_z, n_x = n_fs // n_y, n_tp // 2
    n_q = n_z // 2
    f, t = lax.axis_index("fs"), lax.axis_index("tp")
    z, y, x, c = f // n_y, f % n_y, t // 2, t % 2
    q, h = z // 2, z % 2
    rows, d_model = tokens.shape
    depth, half = w_gate.shape[0], w_gate.shape[1] // 2
    piece = rows // n_tp

    def to_z(a, step):
        return lax.ppermute(a, "fs", [(i, (i + step * n_y) % n_fs) for i in range(n_fs)])

    def to_y(a, step):
        return lax.ppermute(
            a, "fs", [(i, i // n_y * n_y + (i + step) % n_y) for i in range(n_fs)]
        )

    def to_twin(a):
        return lax.ppermute(
            a, "fs", [(i, (i // n_y ^ 1) * n_y + i % n_y) for i in range(n_fs)]
        )

    def to_x(a, step):
        return lax.ppermute(a, "tp", [(i, (i + 2 * step) % n_tp) for i in range(n_tp)])

    def to_core(a):
        return lax.ppermute(a, "tp", [(i, i ^ 1) for i in range(n_tp)])

    mine = jnp.stack(
        [lax.dynamic_slice_in_dim(a, t * piece, piece, 0) for a in (tokens, cotangent)]
    )
    down_t = w_down.T

    def half_of(which):
        gate_up = jnp.concatenate(
            [lax.dynamic_slice_in_dim(w, which * half, half, 1) for w in (w_gate, w_up)], axis=1
        )
        return gate_up, lax.dynamic_slice_in_dim(down_t, which * half, half, 1)

    own, other = half_of(h), half_of(1 - h)

    w_gu, w_dn, got = gather_all(n_z, n_y, n_x, own, other, mine)
    w_gu, w_dn = w_gu.reshape(d_model, 2 * half), w_dn.reshape(d_model, half)
    got = got.reshape(2, rows, d_model)
    tokens2 = jnp.concatenate([tokens, got[0]], axis=0)
    cot2 = jnp.concatenate([cotangent, got[1]], axis=0)

    xf = tokens2.astype(F32)
    inv = lax.rsqrt(jnp.mean(xf * xf, axis=-1, keepdims=True) + EPS)
    normed = (xf * inv * norm_gain).astype(BF16)
    gate_up = jnp.dot(normed, w_gu, preferred_element_type=F32)
    gate, up = gate_up[:, :half], gate_up[:, half:]
    sig = jax.nn.sigmoid(gate)
    act = gate * sig
    hidden = (act * up).astype(BF16)

    share = 0.5 * lax.dot_general(
        cot2, hidden, (((0,), (0,)), ((), ())), preferred_element_type=F32
    )
    share = share.reshape(n_q, 2, n_y, depth, half)
    share, w_dn = lax.optimization_barrier((share, w_dn))

    def sent_over_y(pair):
        block = take(share, pair)
        return [to_y(take(block, (y + s) % n_y, 1).astype(BF16), s) for s in range(1, n_y)]

    def over_y(pair, came):
        return sum([a.astype(F32) for a in came], take(take(share, pair), y, 1))

    first = [sent_over_y((q + s) % n_q) for s in range(1, n_q)]

    d_hidden = 0.5 * jnp.dot(cot2, w_dn, preferred_element_type=F32)
    d_gate = (d_hidden * up * sig * (1.0 + gate * (1.0 - sig))).astype(BF16)
    d_up = (d_hidden * act).astype(BF16)
    d_both = jnp.concatenate([d_gate, d_up], axis=1)
    part = lax.dot_general(
        d_both, w_gu, (((1,), (1,)), ((), ())), preferred_element_type=F32
    )
    part, first = lax.optimization_barrier((part.astype(BF16), first))

    away = [
        to_z(over_y((q + s) % n_q, first[s - 1]).astype(BF16), 2 * s) for s in range(1, n_q)
    ]
    total = over_y(q, sent_over_y(q))
    total = sum([a.astype(F32) for a in away], total)
    kept = take(total, h)
    came = to_twin(take(total, 1 - h).astype(BF16)).astype(F32)
    grad_down = place([(h, kept.T), (1 - h, came.T)], 2).reshape(2 * half, depth)
    norms = jnp.sum(grad_down * grad_down, axis=1)
    norms = sum([to_y(norms, s) for s in range(1, n_y)], norms)
    down_norms = sum([to_z(norms, s) for s in range(1, n_z)], norms)

    part = part.reshape(2, n_x, 2, piece, d_model)
    part = take(part, c, 2).astype(F32) + to_core(take(part, 1 - c, 2)).astype(F32)
    total = take(part, x, 1)
    for s in range(1, n_x):
        total = total + to_x(take(part, (x + s) % n_x, 1).astype(BF16), s).astype(F32)
    d_normed = total[0] + to_twin(total[1].astype(BF16)).astype(F32)

    xp = lax.dynamic_slice_in_dim(tokens, t * piece, piece, 0).astype(F32)
    inv_p = lax.rsqrt(jnp.mean(xp * xp, axis=-1, keepdims=True) + EPS)
    scaled = xp * inv_p
    d_scaled = d_normed * norm_gain
    inner = jnp.mean(d_scaled * scaled, axis=-1, keepdims=True)
    grad = (inv_p * (d_scaled - scaled * inner)).astype(BF16)
    grad = place([(x, grad)] + [((x - s) % n_x, to_x(grad, s)) for s in range(1, n_x)], n_x)
    grad = place([(c, grad), (1 - c, to_core(grad))], 2)
    grad_tokens = grad.transpose(1, 0, 2, 3).reshape(rows, d_model)
    return (grad_tokens, grad_down, down_norms)


def solution(mesh):
    in_specs = (P("fs", None), P(), P("fs", "tp"), P("fs", "tp"), P("tp", "fs"), P("fs", None))
    out_specs = (P("fs", None), P("tp", "fs"), P("tp"))
    return jax.shard_map(
        functools.partial(shards, mesh.shape["fs"], mesh.shape["tp"]),
        mesh=mesh, in_specs=in_specs, out_specs=out_specs, check_vma=False,
    )
```
